512 devices in a mesh: ep: 32 (over z, core), tp: 16 (over y, x).
Axes of the slice: x: 4, y: 4, z: 16, core: 2. Of those that a mesh axis runs over, the one named last changes fastest.
Arguments:
- residual: bfloat16 [2048, 2048], P('ep', 'tp')
- state_re: float32 [2048, 64, 64], P('ep', 'tp'), may hold values from -4 to 4
- state_im: float32 [2048, 64, 64], P('ep', 'tp'), may hold values from -4 to 4
- mix_gain: float32 [2048], replicated, may hold values from 0.1 to 1.9
- proj_in: bfloat16 [2048, 1024], P(None, 'tp'), may hold values from -0.125 to 0.125
- decay_rate: float32 [64, 64], P('tp'), may hold values from 0.1 to 10
- frequency: float32 [64, 64], P('tp'), may hold values from 0 to 201.06177
- log_step: float32 [64], P('tp'), may hold values from -6.9078 to -2.3026
- input_re: float32 [64, 64, 16], P('tp'), may hold values from -1 to 1
- input_im: float32 [64, 64, 16], P('tp'), may hold values from -1 to 1
- read_re: float32 [64, 16, 64], P('tp'), may hold values from -0.5 to 0.5
- read_im: float32 [64, 16, 64], P('tp'), may hold values from -0.5 to 0.5
- skip_gain: float32 [1024], P('tp'), may hold values from -4 to 4
- glu_weight: bfloat16 [1024, 1024], P(None, 'tp'), may hold values from -0.1875 to 0.1875
- out_proj: bfloat16 [1024, 2048], P(None, 'tp'), may hold values from -0.1875 to 0.1875
- ffn_gain: float32 [2048], replicated, may hold values from 0.1 to 1.9
- router: float32 [2048, 32], replicated, may hold values from -0.125 to 0.125
- gate_weight: bfloat16 [32, 2048, 4096], P('ep', None, 'tp'), may hold values from -0.33007812 to 0.33007812
- up_weight: bfloat16 [32, 2048, 4096], P('ep', None, 'tp'), may hold values from -0.33007812 to 0.33007812
- down_weight: bfloat16 [32, 4096, 2048], P('ep', 'tp'), may hold values from -0.046875 to 0.046875
- route_ids: int32 [2048, 4], P('ep'), may hold values from 0 to 31, all different within a row; in each aligned block of 64 rows (0 to 63, 64 to 127, ...) at most 9 rows name the same one
Outputs:
- layer_out: bfloat16 [2048, 2048], P('ep', 'tp')
- state_re_new: float32 [2048, 64, 64], P('ep', 'tp')
- state_im_new: float32 [2048, 64, 64], P('ep', 'tp')
The draws below stay inside these ranges and needn't reach their ends.
Inputs may be any that keep to these rules, and one draw needn't show every extreme that they name: `route_ids`: each row names 4 different experts. Within the rows of one ep index (aligned blocks of 64 rows) no expert is named more than 9 times, and in some block some expert is named exactly 9 times.
All inputs are finite; a program needn't handle non-finite values.
Results may differ from the reference program's by a relative error of at most 0.014.
Values may be sent and summed in bfloat16 or wider, within the bound.
No kernel may reach another device: no remote copies, remote signals or barrier semaphores. Data moves between devices by JAX's collectives and lax.ppermute only.
A program may use at most 64 MiB of HBM per device.

```python
import math
import jax
import jax.numpy as jnp
import numpy as np
from jax import lax

D = 2048
GROUPS = 64
GROUP_CH = 16
STATE = 64
FF = 4096
TOPK = 4
SEQ_DEV = 64
CH = 1024
EXPERTS = 32
SEQS = 2048
CAP = 9
N_EP = 32
N_TP = 16


def draw_residual(key, part):
    key_base = jax.random.fold_in(key, 11)
    key_rows = jax.random.fold_in(key, 12)
    column = jnp.arange(D, dtype=jnp.float32) / D
    row_scale = jnp.exp(jax.random.uniform(key_rows, (SEQS, 1), jnp.float32, math.log(0.3), math.log(3.0)))
    base = jax.random.normal(key_base, (SEQS, D), jnp.float32)
    col_scale = 0.3 * jnp.exp(column * math.log(10.0))
    values = base * row_scale * col_scale[None, :]
    return values.astype(jnp.bfloat16)


def strengthened(array, own_key, source, target, shards_of, factor):
    owner, partner = [(jnp.arange(array.shape[axis_at]) // (array.shape[axis_at] // shards_of)).reshape([-1 if axis == axis_at else 1 for axis in range(array.ndim)]) for axis_at in (source, target)]
    chosen = jax.random.permutation(own_key, shards_of)[partner]
    strong = (owner == chosen) | (owner == (partner + shards_of // 2) % shards_of)
    return jnp.where(strong, factor * array, array)


def block_scale(key, shape, split, smallest, high):
    level, own = 1.0, jax.random.fold_in(key, 6)
    for dim, blocks in split:
        draws = jnp.exp(jax.random.uniform(jax.random.fold_in(own, dim), (blocks,), jnp.float32, smallest / len(split), high / len(split)))
        level = level * jnp.repeat(draws, shape[dim] // blocks).reshape([-1 if axis == dim else 1 for axis in range(len(shape))])
    return level


def assign_block(stream_key, own, number, rows, count, top, limit, skew):
    order = jax.random.permutation(stream_key, count)
    crowded, usual = load_shares(count, rows * top, limit, skew, True), load_shares(count, rows * top, limit, skew, False)
    places = jnp.arange(count)

    def named(sizes, turn):
        used = int((sizes > 0).sum())
        fixed = max(1, used // 4)
        passed = fixed + (places - fixed + turn * (used - fixed)) % max(1, count - fixed)
        return jnp.zeros((count,), jnp.int32).at[order[jnp.where(places < fixed, places, passed)]].set(jnp.asarray(sizes, jnp.int32))

    sizes = jnp.where(number % 4 == 0, named(crowded, number // 4), named(usual, number - number // 4 - 1))
    mixed = jax.random.permutation(jax.random.fold_in(own, 3), count)
    giver, receiver = mixed[0:count // 2 * 2:2], mixed[1:count // 2 * 2:2]
    margin = jnp.minimum(sizes[giver] - 1, limit - sizes[receiver]) // 2
    margin = jnp.where((giver == order[0]) | (receiver == order[0]) | (sizes[receiver] == 0), 0, jnp.maximum(margin, 0))
    passed = jax.random.randint(jax.random.fold_in(own, 4), (count // 2,), 0, 1 << 20) % (margin + 1)
    sizes = sizes.at[giver].add(-passed).at[receiver].add(passed)
    items = jnp.searchsorted(jnp.cumsum(sizes), jnp.arange(rows * top), side="right").astype(jnp.int32)
    listing = items.reshape(top, rows).T
    listing = listing[jax.random.permutation(jax.random.fold_in(own, 1), rows)]
    turn = jax.random.randint(jax.random.fold_in(own, 2), (rows, 1), 0, top)
    return jnp.take_along_axis(listing, (jnp.arange(top)[None, :] + turn) % top, axis=1)


def load_shares(number_of, total, reach, skew, full):
    weights = [(1 << 20) // math.isqrt(rank ** skew) + 1 for rank in range(1, number_of + 1)]
    largest = reach if full else min(reach, max(-(-total // number_of), total * weights[0] // sum(weights)))
    least = 1 if total - largest >= number_of - 1 else 0
    holding, spare = [largest] + [least] * (number_of - 1), total - largest - least * (number_of - 1)
    while spare > 0:
        movable = [i for i in range(1, number_of) if holding[i] < largest] or [i for i in range(1, number_of) if holding[i] < reach]
        mass, left = sum([weights[i] for i in movable]), spare
        for i in movable:
            more = min(reach - holding[i], max(1, left * weights[i] // mass), spare)
            holding[i] = holding[i] + more
            spare = spare - more
    return np.array(holding)


def centred(key, shape, width, reach, cuts=(), held_as=jnp.bfloat16):
    gain = block_scale(key, shape, cuts, -0.22, 0.18) if cuts else 1.0
    entries = jax.random.normal(key, shape, jnp.float32) * width * gain
    return jnp.minimum(jnp.maximum(entries, -reach), reach).astype(held_as)


def heavy_noise(stream_key, shape, scale, bound, split, heavy, held_as=jnp.bfloat16):
    drawn = scale * jax.random.normal(stream_key, shape, jnp.float32)
    if split:
        drawn = drawn * block_scale(stream_key, shape, split, -0.22, 0.18)
    return jnp.clip(strengthened(drawn, jax.random.fold_in(stream_key, 3), *heavy), -bound, bound).astype(held_as)


def setup_inputs(seed: int = 0) -> dict:
    arg_keys = jax.random.split(jax.random.key(seed), 22)
    residual = draw_residual(jax.random.fold_in(arg_keys[21], 71), 0)
    state_re = centred(arg_keys[1], (SEQS, GROUPS, STATE), 0.5, 4.0, ((0, 32), (1, 16)), jnp.float32)
    state_im = centred(arg_keys[2], (SEQS, GROUPS, STATE), 0.5, 4.0, ((0, 32), (1, 16)), jnp.float32)
    mix_gain = jnp.clip(1.0 + 0.18 * jax.random.normal(arg_keys[3], (D,), jnp.float32), 0.1, 1.9)
    proj_in = centred(arg_keys[4], (D, CH), D ** -0.5, 0.125, ((1, 16),))
    decay_rate = jnp.clip(jnp.exp(math.log(10.0) - 4.6051702 * jax.random.uniform(arg_keys[5], (GROUPS, STATE), jnp.float32) ** block_scale(arg_keys[5], (GROUPS, STATE), ((0, 16),), -0.2, 0.2)), 0.1, 10.0)
    frequency = jnp.clip(201.06177 * jax.random.uniform(arg_keys[6], (GROUPS, STATE), jnp.float32) ** block_scale(arg_keys[6], (GROUPS, STATE), ((0, 16),), -0.2, 0.2), 0.0, 201.06177)
    log_step = jnp.clip(-6.9078 + 4.6052003 * jax.random.uniform(arg_keys[7], (GROUPS,), jnp.float32) ** block_scale(arg_keys[7], (GROUPS,), ((0, 16),), -0.2, 0.2), -6.9078, -2.3026)
    input_re = centred(arg_keys[8], (GROUPS, STATE, GROUP_CH), (2 * GROUP_CH) ** -0.5, 1.0, ((0, 16),), jnp.float32)
    input_im = centred(arg_keys[9], (GROUPS, STATE, GROUP_CH), (2 * GROUP_CH) ** -0.5, 1.0, ((0, 16),), jnp.float32)
    read_re = centred(arg_keys[10], (GROUPS, GROUP_CH, STATE), (2 * STATE) ** -0.5, 0.5, ((0, 16),), jnp.float32)
    read_im = centred(arg_keys[11], (GROUPS, GROUP_CH, STATE), (2 * STATE) ** -0.5, 0.5, ((0, 16),), jnp.float32)
    skip_gain = centred(arg_keys[12], (CH,), 1.0, 4.0, ((0, 16),), jnp.float32)
    glu_weight = centred(arg_keys[13], (CH, CH), CH ** -0.5, 0.1875, ((1, 16),))
    out_proj = centred(arg_keys[14], (CH, D), CH ** -0.5, 0.1875, ((1, 16),))
    ffn_gain = jnp.clip(1.0 + 0.18 * jax.random.normal(arg_keys[15], (D,), jnp.float32), 0.1, 1.9)
    router = centred(arg_keys[16], (D, EXPERTS), D ** -0.5, 0.125, (), jnp.float32)
    gate_weight = centred(arg_keys[17], (EXPERTS, D, FF), (2.5 * D ** -0.5), 0.33007812, ((0, 32), (2, 16)))
    up_weight = centred(arg_keys[18], (EXPERTS, D, FF), (2.5 * D ** -0.5), 0.33007812, ((0, 32), (2, 16)))
    down_weight = heavy_noise(arg_keys[19], (EXPERTS, FF, D), (8 * FF) ** -0.5, 0.046875, ((0, 32), (1, 16)), (1, 2, 16, 2.0))
    route_ids_keys = jax.random.split(jax.random.fold_in(arg_keys[20], 1), SEQS // SEQ_DEV)
    route_ids_turns = jax.random.permutation(jax.random.fold_in(arg_keys[20], 3), SEQS // SEQ_DEV)
    route_ids = jax.vmap(lambda own, number: assign_block(jax.random.fold_in(arg_keys[20], 2), own, number, SEQ_DEV, EXPERTS, TOPK, CAP, 1))(route_ids_keys, route_ids_turns).reshape((SEQS, TOPK))
    return {"residual": residual, "state_re": state_re, "state_im": state_im, "mix_gain": mix_gain, "proj_in": proj_in, "decay_rate": decay_rate, "frequency": frequency, "log_step": log_step, "input_re": input_re, "input_im": input_im, "read_re": read_re, "read_im": read_im, "skip_gain": skip_gain, "glu_weight": glu_weight, "out_proj": out_proj, "ffn_gain": ffn_gain, "router": router, "gate_weight": gate_weight, "up_weight": up_weight, "down_weight": down_weight, "route_ids": route_ids}


EPSILON = 1e-05
LIMIT = 7.0
ALPHA = 1.702

def discretise(decay_rate, frequency, log_step, input_re, input_im):
    real_part = -decay_rate
    imag_part = frequency
    step_size = jnp.exp(log_step)[:, None]
    magnitude = jnp.exp(step_size * real_part)
    abar_re = magnitude * jnp.cos(step_size * imag_part)
    abar_im = magnitude * jnp.sin(step_size * imag_part)
    denom = real_part * real_part + imag_part * imag_part
    minus_one = abar_re - 1.0
    coef_re = (minus_one * real_part + abar_im * imag_part) / denom
    coef_im = (abar_im * real_part - minus_one * imag_part) / denom
    bbar_re = coef_re[..., None] * input_re - coef_im[..., None] * input_im
    bbar_im = coef_re[..., None] * input_im + coef_im[..., None] * input_re
    return (abar_re, abar_im, bbar_re, bbar_im)

def expert_rows(operands):
    tokens, w_gate, w_up, w_down = operands
    gate_pre = jnp.dot(tokens, w_gate, preferred_element_type=jnp.float32)
    up_pre = jnp.dot(tokens, w_up, preferred_element_type=jnp.float32)
    gate_cl = jnp.minimum(gate_pre, LIMIT)
    up_cl = jnp.clip(up_pre, -LIMIT, LIMIT)
    active = ((up_cl + 1.0) * (gate_cl * jax.nn.sigmoid(ALPHA * gate_cl))).astype(jnp.bfloat16)
    rows = active.shape[0]
    block = FF // N_TP
    act_blocks = active.astype(jnp.float32).reshape(rows, N_TP, block)
    down_blocks = w_down.astype(jnp.float32).reshape(N_TP, block, D)
    partial_value = jnp.einsum('rtf,tfd->trd', act_blocks, down_blocks).astype(jnp.bfloat16)
    return lax.optimization_barrier(jnp.sum(partial_value.astype(jnp.float32), axis=0)).astype(jnp.bfloat16)

def reference(residual, state_re, state_im, mix_gain, proj_in, decay_rate, frequency, log_step, input_re, input_im, read_re, read_im, skip_gain, glu_weight, out_proj, ffn_gain, router, gate_weight, up_weight, down_weight, route_ids):
    high = lax.Precision.HIGHEST
    resid_f = residual.astype(jnp.float32)
    scale_one = lax.rsqrt(lax.optimization_barrier(jnp.mean(resid_f * resid_f, axis=1, keepdims=True)) + EPSILON)
    xnorm = (resid_f * scale_one * mix_gain).astype(jnp.bfloat16)
    mix_in = jnp.dot(xnorm, proj_in, preferred_element_type=jnp.float32).astype(jnp.bfloat16)
    mix_f = mix_in.astype(jnp.float32)
    grouped = mix_f.reshape(SEQS, GROUPS, GROUP_CH)
    abar_re, abar_im, bbar_re, bbar_im = discretise(decay_rate, frequency, log_step, input_re, input_im)
    drive_re = jnp.einsum('sgc,gnc->sgn', grouped, bbar_re, precision=high)
    drive_im = jnp.einsum('sgc,gnc->sgn', grouped, bbar_im, precision=high)
    state_re_new = abar_re * state_re - abar_im * state_im + drive_re
    state_im_new = abar_re * state_im + abar_im * state_re + drive_im
    readout = jnp.einsum('sgn,gcn->sgc', state_re_new, read_re, precision=high) - jnp.einsum('sgn,gcn->sgc', state_im_new, read_im, precision=high)
    mixer = jax.nn.gelu(readout.reshape(SEQS, CH) + skip_gain * mix_f, approximate=False)
    glu_gate = jnp.dot(mixer.astype(jnp.bfloat16), glu_weight, preferred_element_type=jnp.float32)
    gated = (mixer * jax.nn.sigmoid(glu_gate)).astype(jnp.bfloat16)
    mixed = jnp.dot(gated, out_proj, preferred_element_type=jnp.float32)
    stream = (resid_f + mixed).astype(jnp.bfloat16)
    stream_f = stream.astype(jnp.float32)
    inverse = lax.rsqrt(lax.optimization_barrier(jnp.mean(stream_f * stream_f, axis=1, keepdims=True)) + EPSILON)
    normed = (stream_f * inverse * ffn_gain).astype(jnp.bfloat16)
    logits = jnp.dot(stream_f * ffn_gain, router, precision=high) * inverse
    picked = jnp.take_along_axis(logits, route_ids, axis=1)
    expon = jnp.exp(picked)
    weights = expon / lax.optimization_barrier(jnp.sum(expon, axis=1, keepdims=True))
    flat_route = route_ids.reshape(N_EP, SEQ_DEV * TOPK).astype(jnp.int32)
    one_hot = (flat_route[..., None] == jnp.arange(EXPERTS, dtype=jnp.int32)).astype(jnp.int32)
    before = jnp.cumsum(one_hot, axis=1) - one_hot
    slot_ids = lax.optimization_barrier(jnp.sum(before * one_hot, axis=2)).astype(jnp.int32)
    source = jnp.broadcast_to(jnp.arange(N_EP, dtype=jnp.int32)[:, None], flat_route.shape)
    tokens = jnp.broadcast_to(normed.reshape(N_EP, SEQ_DEV, 1, D), (N_EP, SEQ_DEV, TOPK, D))
    tokens = tokens.reshape(N_EP, SEQ_DEV * TOPK, D)
    buffer = jnp.zeros((EXPERTS, N_EP, CAP, D), jnp.bfloat16)
    buffer = buffer.at[flat_route, source, slot_ids].set(tokens)
    results = lax.map(expert_rows, (buffer.reshape(EXPERTS, N_EP * CAP, D), gate_weight, up_weight, down_weight))
    results = results.reshape(EXPERTS, N_EP, CAP, D)
    fetched = results[flat_route, source, slot_ids].astype(jnp.float32).reshape(SEQS, TOPK, D)
    experts_sum = lax.optimization_barrier(jnp.sum(weights[..., None] * fetched, axis=1))
    layer_out = (stream_f + experts_sum).astype(jnp.bfloat16)
    return (layer_out, state_re_new, state_im_new)
```

```python
import functools

import jax
import jax.numpy as jnp
from jax import lax
from jax.experimental import pallas as pl
from jax.experimental.pallas import tpu as pltpu
from jax.sharding import Mesh
from jax.sharding import PartitionSpec as P

TP = ("tp_0", "tp_1")
EPSILON = 1e-05
LIMIT = 7.0
ALPHA = 1.702
F32 = jnp.float32
BF16 = jnp.bfloat16
TILE = 128


def call(body, out, *args, mib=16, **settings):
    return pl.pallas_call(
        body,
        out_shape=out,
        compiler_params=pltpu.CompilerParams(vmem_limit_bytes=mib << 20),
        **settings,
    )(*args)


def shape_of(shape, dtype):
    return jax.ShapeDtypeStruct(shape, dtype)


def halves(value):
    high = value.astype(BF16)
    return high, (value - high.astype(F32)).astype(BF16)


def dot(left, right):
    return jnp.dot(left, right, preferred_element_type=F32)


def dot_rows(left, right):
    return lax.dot_general(left, right, (((1,), (1,)), ((), ())), preferred_element_type=F32)


def exchange(blocks, axis):
    return lax.all_to_all(blocks, axis, 0, 0, tiled=True)


def discretise(decay_rate, frequency, log_step, input_re, input_im):
    real_part = -decay_rate
    step_size = jnp.exp(log_step)[:, None]
    magnitude = jnp.exp(step_size * real_part)
    abar_re = magnitude * jnp.cos(step_size * frequency)
    abar_im = magnitude * jnp.sin(step_size * frequency)
    denom = real_part * real_part + frequency * frequency
    minus_one = abar_re - 1.0
    coef_re = (minus_one * real_part + abar_im * frequency) / denom
    coef_im = (abar_im * real_part - minus_one * frequency) / denom
    bbar_re = coef_re[:, None] * input_re - coef_im[:, None] * input_im
    bbar_im = coef_re[:, None] * input_im + coef_im[:, None] * input_re
    return (abar_re, abar_im, bbar_re, bbar_im)


def block_diagonal(blocks):
    count, rows, cols = blocks.shape
    flat = blocks.reshape(count * rows, cols)
    wide = jnp.concatenate([flat] * count, axis=1)
    row_block = lax.broadcasted_iota(jnp.int32, wide.shape, 0) // rows
    col_block = lax.broadcasted_iota(jnp.int32, wide.shape, 1) // cols
    return jnp.where(row_block == col_block, wide, 0.0)


def packed(value):
    half = value.shape[0] // 2
    return jnp.concatenate([value[:half], value[half:]], axis=1)


def unpacked(ref):
    peers, half, lanes = ref.shape
    width = lanes // 2
    left = lax.broadcasted_iota(jnp.int32, (half, lanes), 1) < width
    top, bottom = [], []
    for pair in range(peers // 2):
        one = ref[2 * pair].astype(F32)
        two = ref[2 * pair + 1].astype(F32)
        top.append(jnp.where(left, one, pltpu.roll(two, width, 1)))
        bottom.append(jnp.where(left, pltpu.roll(one, width, 1), two))
    rows = [jnp.concatenate(top, axis=1), jnp.concatenate(bottom, axis=1)]
    return jnp.concatenate(rows, axis=0).astype(BF16)


def routing_kernel(per, cap, experts, route_ref, across_ref, place_ref, fetch_ref, pick_ref, keep_ref, grow_ref, tag_ref):
    seqs, top = route_ref.shape
    slots = place_ref.shape[0]
    rows = keep_ref.shape[0]
    route = route_ref[...]
    across = across_ref[...]

    def iota(shape, dim):
        return lax.broadcasted_iota(jnp.int32, shape, dim)

    expert_lane = iota((seqs, experts), 1)
    expert_row = iota((experts, seqs), 0)
    named = sum((route[:, k : k + 1] == expert_lane).astype(F32) for k in range(top))
    named_across = sum((across[k : k + 1, :] == expert_row).astype(F32) for k in range(top))
    earlier = (iota((seqs, seqs), 1) < iota((seqs, seqs), 0)).astype(BF16)
    earlier_across = (iota((seqs, seqs), 0) < iota((seqs, seqs), 1)).astype(BF16)
    count = dot(earlier, named.astype(BF16))
    count_across = dot(named_across.astype(BF16), earlier_across)
    slot_row = iota((slots, seqs), 0)
    slot_lane = iota((seqs, slots), 1)
    lane = iota((seqs, TILE), 1)
    place = jnp.zeros((slots, seqs), F32)
    for k in range(top):
        chosen = route[:, k : k + 1]
        slot = jnp.sum(jnp.where(chosen == expert_lane, count, 0.0), axis=1, keepdims=True).astype(jnp.int32)
        fetch_ref[k * seqs : (k + 1) * seqs, :] = (slot_lane == chosen * per + slot).astype(F32).astype(BF16)
        fetch_ref[(top + k) * seqs : (top + k + 1) * seqs, :] = (
            (slot_lane == chosen * per + cap).astype(F32).astype(BF16)
        )
        pick_ref[k * seqs : (k + 1) * seqs, :] = ((lane == slot) | (lane == slot + 16)).astype(F32)
        chosen_across = across[k : k + 1, :]
        slot_across = jnp.sum(
            jnp.where(chosen_across == expert_row, count_across, 0.0), axis=0, keepdims=True
        ).astype(jnp.int32)
        place = place + (slot_row == chosen_across * per + slot_across).astype(F32)
    place_ref[...] = place.astype(BF16)
    row = iota((rows, slots), 0)
    keep_ref[...] = (iota((rows, slots), 1) == row + ninth(row)).astype(F32).astype(BF16)
    col = iota((slots, rows), 1)
    grow_ref[...] = (iota((slots, rows), 0) == col + ninth(col)).astype(F32).astype(BF16)
    tag_ref[...] = (iota((slots, rows), 0) == ninth(col) * per + cap).astype(F32).astype(BF16)


def ninth(value):
    return (value * 7282) >> 16


def mixer_kernel(
    resid_ref, gain_ref, proj_ref, state_re_ref, state_im_ref, abar_re_ref, abar_im_ref,
    input_re_ref, input_im_ref, read_re_ref, read_im_ref, skip_ref,
    new_re_ref, new_im_ref, mixer_ref, send_ref,
):
    peers, seqs, cols = resid_ref.shape
    square = jnp.zeros((seqs, cols), F32)
    for t in range(peers):
        part = resid_ref[t].astype(F32)
        square = square + part * part
    mean = jnp.sum(square, axis=1, keepdims=True) / (peers * cols)
    scale = lax.rsqrt(mean + EPSILON)
    normed = jnp.concatenate(
        [(resid_ref[t].astype(F32) * scale * gain_ref[t : t + 1, :]).astype(BF16) for t in range(peers)], axis=1
    )
    mix = dot_rows(normed, proj_ref[...]).astype(BF16)
    width = state_re_ref.shape[1]

    def driven(ref):
        high, low = halves(ref[...])
        return dot(mix, high) + dot(mix, low)

    old_re, old_im = state_re_ref[...], state_im_ref[...]
    abar_re, abar_im = abar_re_ref[...], abar_im_ref[...]
    new_re = abar_re * old_re - abar_im * old_im + driven(input_re_ref)
    new_im = abar_re * old_im + abar_im * old_re + driven(input_im_ref)
    new_re_ref[...] = new_re
    new_im_ref[...] = new_im

    def read(value, ref):
        high, low = halves(value)
        read_high, read_low = halves(ref[...])
        return dot_rows(high, read_high) + dot_rows(high, read_low) + dot_rows(low, read_high)

    value = read(new_re, read_re_ref) - read(new_im, read_im_ref) + skip_ref[...] * mix.astype(F32)
    mixer = 0.5 * value * (1.0 + lax.erf(value * 0.7071067811865476))
    mixer_ref[...] = mixer
    sent = packed(mixer).astype(BF16)
    for t in range(peers):
        send_ref[t] = sent


def gate_kernel(all_ref, weight_ref, mixer_ref, send_ref):
    gate = dot_rows(unpacked(all_ref), weight_ref[...])
    gated = packed(mixer_ref[...] * jax.nn.sigmoid(gate)).astype(BF16)
    for t in range(send_ref.shape[0]):
        send_ref[t] = gated


def stream_kernel(all_ref, weight_ref, resid_ref, place_ref, stream_ref, send_ref):
    mixed = dot(unpacked(all_ref), weight_ref[...])
    stream = (resid_ref[...].astype(F32) + mixed).astype(BF16)
    stream_ref[...] = stream
    send_ref[...] = dot(place_ref[...], stream).astype(BF16)


def spread_kernel(arrived_ref, keep_ref, send_ref):
    tokens = dot(keep_ref[...], arrived_ref[...]).astype(BF16)
    for t in range(send_ref.shape[0]):
        send_ref[t] = tokens


def inverse_of(tokens_ref):
    peers, rows, cols = tokens_ref.shape
    square = jnp.zeros((rows, cols), F32)
    for t in range(peers):
        part = tokens_ref[t].astype(F32)
        square = square + part * part
    return lax.rsqrt(jnp.sum(square, axis=1, keepdims=True) / (peers * cols) + EPSILON)


def expert_kernel(tokens_ref, gain_ref, gate_ref, up_ref, down_ref, out_ref):
    peers, rows, cols = tokens_ref.shape
    inverse = inverse_of(tokens_ref)
    normed = jnp.concatenate(
        [(tokens_ref[t].astype(F32) * inverse * gain_ref[t : t + 1, :]).astype(BF16) for t in range(peers)], axis=1
    )
    gate = jnp.minimum(dot(normed, gate_ref[0]), LIMIT)
    up = jnp.clip(dot(normed, up_ref[0]), -LIMIT, LIMIT)
    active = ((up + 1.0) * (gate * jax.nn.sigmoid(ALPHA * gate))).astype(BF16)
    for t in range(0, peers, 2):
        part = dot(active, down_ref[0, :, t * cols : (t + 2) * cols]).astype(BF16)
        out_ref[t] = part[:, :cols]
        out_ref[t + 1] = part[:, cols:]


def logit_kernel(tokens_ref, gain_ref, router_ref, tag_ref, out_ref):
    peers, rows, cols = tokens_ref.shape
    inverse = inverse_of(tokens_ref)
    total = jnp.zeros((rows, cols), F32)
    for t in range(peers):
        total = total + tokens_ref[t].astype(F32) * gain_ref[t : t + 1, :] * router_ref[t : t + 1, :]
    logit = jnp.sum(total, axis=1, keepdims=True) * inverse
    high, low = halves(logit)
    row = lax.broadcasted_iota(jnp.int32, (rows, TILE), 0)
    place = row - 9 * ninth(row)
    lane = lax.broadcasted_iota(jnp.int32, (rows, TILE), 1)
    marked = jnp.where(lane == place, high.astype(F32), 0.0) + jnp.where(lane == place + 16, low.astype(F32), 0.0)
    out_ref[...] = dot(tag_ref[...], marked.astype(BF16)).astype(BF16)


def return_kernel(parts_ref, grow_ref, logits_ref, send_ref):
    total = parts_ref[0].astype(F32)
    for t in range(1, parts_ref.shape[0]):
        total = total + parts_ref[t].astype(F32)
    grown = dot(grow_ref[...], total.astype(BF16))
    send_ref[...] = (grown + logits_ref[...].astype(F32)).astype(BF16)


def combine_kernel(top, back_ref, fetch_ref, pick_ref, stream_ref, out_ref):
    fetched = dot(fetch_ref[...], back_ref[...])
    seqs = stream_ref.shape[0]
    half = top * seqs
    picked = jnp.sum(fetched[half:] * pick_ref[...], axis=1, keepdims=True)
    expon = jnp.exp(picked)
    values = [fetched[k * seqs : (k + 1) * seqs] for k in range(top)]
    shares = [expon[k * seqs : (k + 1) * seqs] for k in range(top)]
    total = functools.reduce(jnp.add, shares)
    mixed = functools.reduce(jnp.add, [(share / total) * value for share, value in zip(shares, values)])
    out_ref[...] = (stream_ref[...].astype(F32) + mixed).astype(BF16)


def per_device(
    residual, state_re, state_im, mix_gain, proj_in, decay_rate, frequency, log_step, input_re, input_im,
    read_re, read_im, skip_gain, glu_weight, out_proj, ffn_gain, router, gate_weight, up_weight, down_weight,
    route_ids,
):
    seqs, cols = residual.shape
    width = mix_gain.shape[0]
    peers = width // cols
    groups, entries = decay_rate.shape
    channels = skip_gain.shape[0]
    ep_size = lax.axis_size("ep")
    experts = router.shape[1]
    top = route_ids.shape[1]
    cap = seqs * top // experts + 1
    per = cap + 1
    slots = ep_size * per
    rows = ep_size * cap
    half = seqs // 2

    all_resid = exchange(jnp.broadcast_to(residual[None], (peers, seqs, cols)), TP)

    place, fetch, pick, keep, grow, tag = call(
        functools.partial(routing_kernel, per, cap, experts),
        (
            shape_of((slots, seqs), BF16), shape_of((2 * top * seqs, slots), BF16), shape_of((top * seqs, TILE), F32),
            shape_of((rows, slots), BF16), shape_of((slots, rows), BF16), shape_of((slots, rows), BF16),
        ),
        route_ids, route_ids.T,
    )
    abar_re, abar_im, bbar_re, bbar_im = discretise(
        decay_rate, frequency, log_step, input_re.transpose(0, 2, 1), input_im.transpose(0, 2, 1)
    )
    lanes = groups * entries
    new_re, new_im, mixer, mixer_send = call(
        mixer_kernel,
        (
            shape_of((seqs, lanes), F32), shape_of((seqs, lanes), F32), shape_of((seqs, channels), F32),
            shape_of((peers, half, 2 * channels), BF16),
        ),
        all_resid, mix_gain.reshape(peers, cols), proj_in.T,
        state_re.reshape(seqs, lanes), state_im.reshape(seqs, lanes),
        abar_re.reshape(1, lanes), abar_im.reshape(1, lanes),
        block_diagonal(bbar_re), block_diagonal(bbar_im), block_diagonal(read_re), block_diagonal(read_im),
        skip_gain.reshape(1, channels),
    )
    all_mixer = exchange(mixer_send, TP)
    gated_send = call(
        gate_kernel, shape_of((peers, half, 2 * channels), BF16), all_mixer, glu_weight.T, mixer
    )
    all_gated = exchange(gated_send, TP)
    stream, token_send = call(
        stream_kernel,
        (shape_of((seqs, cols), BF16), shape_of((slots, cols), BF16)),
        all_gated, out_proj, residual, place,
    )
    arrived = exchange(token_send.reshape(ep_size, per // 2, 2, cols), "ep").reshape(slots, cols)
    tokens_send = call(spread_kernel, shape_of((peers, rows, cols), BF16), arrived, keep)
    tokens = exchange(tokens_send, TP)
    gain = ffn_gain.reshape(peers, cols)
    parts = call(
        expert_kernel, shape_of((peers, rows, cols), BF16), tokens, gain, gate_weight, up_weight, down_weight, mib=24
    )
    own_parts = exchange(parts, TP)
    expert = lax.axis_index("ep")
    own_router = lax.dynamic_slice_in_dim(router.T, expert, 1, 0).reshape(peers, cols)
    logits = call(logit_kernel, shape_of((slots, cols), BF16), tokens, gain, own_router, tag)
    back_send = call(return_kernel, shape_of((slots, cols), BF16), own_parts, grow, logits)
    back = exchange(back_send.reshape(ep_size, per // 2, 2, cols), "ep").reshape(slots, cols)
    layer_out = call(
        functools.partial(combine_kernel, top), shape_of((seqs, cols), BF16), back, fetch, pick, stream
    )
    shape = (seqs, groups, entries)
    return (layer_out, new_re.reshape(shape), new_im.reshape(shape))


def solution(mesh):
    split = Mesh(mesh.devices.reshape(mesh.shape["ep"], 4, 4), ("ep", "tp_0", "tp_1"))
    in_specs = (
        P("ep", TP),
        P("ep", TP, None),
        P("ep", TP, None),
        P(),
        P(None, TP),
        P(TP, None),
        P(TP, None),
        P(TP),
        P(TP, None, None),
        P(TP, None, None),
        P(TP, None, None),
        P(TP, None, None),
        P(TP),
        P(None, TP),
        P(None, TP),
        P(),
        P(),
        P("ep", None, TP),
        P("ep", None, TP),
        P("ep", TP, None),
        P("ep", None),
    )
    out_specs = (P("ep", TP), P("ep", TP, None), P("ep", TP, None))
    return jax.shard_map(
        per_device, mesh=split, in_specs=in_specs, out_specs=out_specs, check_vma=False
    )
```

```python
import functools

import jax
import jax.numpy as jnp
from jax import lax
from jax.experimental import pallas as pl
from jax.experimental.pallas import tpu as pltpu
from jax.sharding import Mesh
from jax.sharding import PartitionSpec as P

TP = ("tp_0", "tp_1")
EPSILON = 1e-05
LIMIT = 7.0
ALPHA = 1.702
F32 = jnp.float32
BF16 = jnp.bfloat16
TILE = 128
STAGGER = 9000


def call(body, out, *args, mib=16, **settings):
    return pl.pallas_call(
        body,
        out_shape=out,
        compiler_params=pltpu.CompilerParams(vmem_limit_bytes=mib << 20),
        **settings,
    )(*args)


def shape_of(shape, dtype):
    return jax.ShapeDtypeStruct(shape, dtype)


def halves(value):
    high = value.astype(BF16)
    return high, (value - high.astype(F32)).astype(BF16)


def dot(left, right):
    return jnp.dot(left, right, preferred_element_type=F32)


def dot_rows(left, right):
    return lax.dot_general(left, right, (((1,), (1,)), ((), ())), preferred_element_type=F32)


def exchange(blocks, axis):
    return lax.all_to_all(blocks, axis, 0, 0, tiled=True)


def discretise(decay_rate, frequency, log_step, input_re, input_im):
    real_part = -decay_rate
    step_size = jnp.exp(log_step)[:, None]
    magnitude = jnp.exp(step_size * real_part)
    abar_re = magnitude * jnp.cos(step_size * frequency)
    abar_im = magnitude * jnp.sin(step_size * frequency)
    denom = real_part * real_part + frequency * frequency
    minus_one = abar_re - 1.0
    coef_re = (minus_one * real_part + abar_im * frequency) / denom
    coef_im = (abar_im * real_part - minus_one * frequency) / denom
    bbar_re = coef_re[:, None] * input_re - coef_im[:, None] * input_im
    bbar_im = coef_re[:, None] * input_im + coef_im[:, None] * input_re
    return (abar_re, abar_im, bbar_re, bbar_im)


def block_diagonal(blocks):
    count, rows, cols = blocks.shape
    flat = jnp.pad(blocks.reshape(count * rows, cols), ((0, 0), (0, TILE - cols)))
    wide = jnp.concatenate([flat] * count, axis=1)
    row_block = lax.broadcasted_iota(jnp.int32, wide.shape, 0) // rows
    col_block = lax.broadcasted_iota(jnp.int32, wide.shape, 1) // TILE
    return jnp.where(row_block == col_block, wide, 0.0)


def packed(value):
    half = value.shape[0] // 2
    return jnp.concatenate([value[:half], value[half:]], axis=1)


def unpacked(ref):
    peers, half, lanes = ref.shape
    width = lanes // 2
    left = lax.broadcasted_iota(jnp.int32, (half, lanes), 1) < width
    top, bottom = [], []
    for pair in range(peers // 2):
        one = ref[2 * pair].astype(F32)
        two = ref[2 * pair + 1].astype(F32)
        top.append(jnp.where(left, one, pltpu.roll(two, width, 1)))
        bottom.append(jnp.where(left, pltpu.roll(one, width, 1), two))
    rows = [jnp.concatenate(top, axis=1), jnp.concatenate(bottom, axis=1)]
    return jnp.concatenate(rows, axis=0).astype(BF16)


def routing_kernel(per, cap, experts, route_ref, across_ref, place_ref, fetch_ref, pick_ref, keep_ref, grow_ref):
    seqs, top = route_ref.shape
    slots = place_ref.shape[0]
    rows = keep_ref.shape[0]
    route = route_ref[...]
    across = across_ref[...]

    def iota(shape, dim):
        return lax.broadcasted_iota(jnp.int32, shape, dim)

    expert_lane = iota((seqs, experts), 1)
    expert_row = iota((experts, seqs), 0)
    named = sum((route[:, k : k + 1] == expert_lane).astype(F32) for k in range(top))
    named_across = sum((across[k : k + 1, :] == expert_row).astype(F32) for k in range(top))
    earlier = (iota((seqs, seqs), 1) < iota((seqs, seqs), 0)).astype(BF16)
    earlier_across = (iota((seqs, seqs), 0) < iota((seqs, seqs), 1)).astype(BF16)
    count = dot(earlier, named.astype(BF16))
    count_across = dot(named_across.astype(BF16), earlier_across)
    slot_row = iota((slots, seqs), 0)
    slot_lane = iota((seqs, slots), 1)
    lane = iota((seqs, TILE), 1)
    place = jnp.zeros((slots, seqs), F32)
    for k in range(top):
        chosen = route[:, k : k + 1]
        slot = jnp.sum(jnp.where(chosen == expert_lane, count, 0.0), axis=1, keepdims=True).astype(jnp.int32)
        fetch_ref[k * seqs : (k + 1) * seqs, :] = (slot_lane == chosen * per + slot).astype(F32).astype(BF16)
        fetch_ref[(top + k) * seqs : (top + k + 1) * seqs, :] = (
            (slot_lane == chosen * per + cap).astype(F32).astype(BF16)
        )
        pick_ref[k * seqs : (k + 1) * seqs, :] = ((lane == slot) | (lane == slot + 16)).astype(F32)
        chosen_across = across[k : k + 1, :]
        slot_across = jnp.sum(
            jnp.where(chosen_across == expert_row, count_across, 0.0), axis=0, keepdims=True
        ).astype(jnp.int32)
        place = place + (slot_row == chosen_across * per + slot_across).astype(F32)
    place_ref[...] = place.astype(BF16)
    row = iota((rows, slots), 0)
    keep_ref[...] = (iota((rows, slots), 1) == row + ninth(row)).astype(F32).astype(BF16)
    col = iota((slots, rows), 1)
    target = iota((slots, rows), 0)
    grow_ref[0] = (target == col + ninth(col)).astype(F32).astype(BF16)
    grow_ref[1] = (target == ninth(col) * per + cap).astype(F32).astype(BF16)


def ninth(value):
    return (value * 7282) >> 16


def mixer_kernel(
    resid_ref, gain_ref, proj_ref, state_re_ref, state_im_ref, abar_re_ref, abar_im_ref,
    input_re_ref, input_im_ref, read_re_ref, read_im_ref, skip_ref,
    new_re_ref, new_im_ref, mixer_ref, send_ref,
):
    peers, seqs, cols = resid_ref.shape
    groups, entries = abar_re_ref.shape
    square = jnp.zeros((seqs, cols), F32)
    for t in range(peers):
        part = resid_ref[t].astype(F32)
        square = square + part * part
    mean = jnp.sum(square, axis=1, keepdims=True) / (peers * cols)
    scale = lax.rsqrt(mean + EPSILON)
    normed = jnp.concatenate(
        [(resid_ref[t].astype(F32) * scale * gain_ref[t : t + 1, :]).astype(BF16) for t in range(peers)], axis=1
    )
    mix = dot_rows(normed, proj_ref[...]).astype(BF16)

    def driven(ref):
        high, low = halves(ref[...])
        return dot(mix, high) + dot(mix, low)

    drive_re, drive_im = driven(input_re_ref), driven(input_im_ref)
    pad = jnp.zeros((seqs, TILE - entries), F32)
    all_re, all_im = [], []
    for g in range(groups):
        old_re, old_im = state_re_ref[:, g, :], state_im_ref[:, g, :]
        abar_re, abar_im = abar_re_ref[g : g + 1, :], abar_im_ref[g : g + 1, :]
        own = slice(g * TILE, g * TILE + entries)
        new_re = abar_re * old_re - abar_im * old_im + drive_re[:, own]
        new_im = abar_re * old_im + abar_im * old_re + drive_im[:, own]
        new_re_ref[:, g, :] = new_re
        new_im_ref[:, g, :] = new_im
        all_re += [new_re, pad]
        all_im += [new_im, pad]

    def read(values, ref):
        high, low = halves(jnp.concatenate(values, axis=1))
        read_high, read_low = halves(ref[...])
        return dot_rows(high, read_high) + dot_rows(high, read_low) + dot_rows(low, read_high)

    value = read(all_re, read_re_ref) - read(all_im, read_im_ref) + skip_ref[...] * mix.astype(F32)
    mixer = 0.5 * value * (1.0 + lax.erf(value * 0.7071067811865476))
    mixer_ref[...] = mixer
    sent = packed(mixer).astype(BF16)
    for t in range(peers):
        send_ref[t] = sent


def gate_kernel(all_ref, weight_ref, mixer_ref, send_ref):
    gate = dot_rows(unpacked(all_ref), weight_ref[...])
    gated = packed(mixer_ref[...] * jax.nn.sigmoid(gate)).astype(BF16)
    for t in range(send_ref.shape[0]):
        send_ref[t] = gated


def stream_kernel(all_ref, weight_ref, resid_ref, place_ref, stream_ref, send_ref):
    mixed = dot(unpacked(all_ref), weight_ref[...])
    stream = (resid_ref[...].astype(F32) + mixed).astype(BF16)
    stream_ref[...] = stream
    send_ref[...] = dot(place_ref[...], stream).astype(BF16)


def spread_kernel(arrived_ref, keep_ref, send_ref):
    tokens = dot(keep_ref[...], arrived_ref[...]).astype(BF16)
    for t in range(send_ref.shape[0]):
        send_ref[t] = tokens
    if STAGGER:
        @pl.when(lax.rem(lax.axis_index("ep"), 2) == 1)
        def _():
            pl.delay(STAGGER)


def expert_kernel(tokens_ref, gain_ref, router_ref, gate_ref, up_ref, down_ref, out_ref, logit_ref):
    peers, rows, cols = tokens_ref.shape
    square = jnp.zeros((rows, cols), F32)
    total = jnp.zeros((rows, cols), F32)
    for t in range(peers):
        part = tokens_ref[t].astype(F32)
        square = square + part * part
        total = total + part * gain_ref[t : t + 1, :] * router_ref[t : t + 1, :]
    inverse = lax.rsqrt(jnp.sum(square, axis=1, keepdims=True) / (peers * cols) + EPSILON)
    high, low = halves(jnp.sum(total, axis=1, keepdims=True) * inverse)
    row = lax.broadcasted_iota(jnp.int32, (rows, TILE), 0)
    place = row - 9 * ninth(row)
    lane = lax.broadcasted_iota(jnp.int32, (rows, TILE), 1)
    marked = jnp.where(lane == place, high.astype(F32), 0.0) + jnp.where(lane == place + 16, low.astype(F32), 0.0)
    logit_ref[...] = marked.astype(BF16)
    normed = jnp.concatenate(
        [(tokens_ref[t].astype(F32) * inverse * gain_ref[t : t + 1, :]).astype(BF16) for t in range(peers)], axis=1
    )
    gate = jnp.minimum(dot(normed, gate_ref[0]), LIMIT)
    up = jnp.clip(dot(normed, up_ref[0]), -LIMIT, LIMIT)
    active = ((up + 1.0) * (gate * jax.nn.sigmoid(ALPHA * gate))).astype(BF16)
    for t in range(0, peers, 2):
        part = dot(active, down_ref[0, :, t * cols : (t + 2) * cols]).astype(BF16)
        out_ref[t] = part[:, :cols]
        out_ref[t + 1] = part[:, cols:]


def return_kernel(parts_ref, grow_ref, logits_ref, send_ref):
    total = parts_ref[0].astype(F32)
    for t in range(1, parts_ref.shape[0]):
        total = total + parts_ref[t].astype(F32)
    grown = dot(grow_ref[0], total.astype(BF16)) + dot(grow_ref[1], logits_ref[...])
    send_ref[...] = grown.astype(BF16)


def combine_kernel(top, back_ref, fetch_ref, pick_ref, stream_ref, out_ref):
    fetched = dot(fetch_ref[...], back_ref[...])
    seqs = stream_ref.shape[0]
    half = top * seqs
    picked = jnp.sum(fetched[half:] * pick_ref[...], axis=1, keepdims=True)
    expon = jnp.exp(picked)
    values = [fetched[k * seqs : (k + 1) * seqs] for k in range(top)]
    shares = [expon[k * seqs : (k + 1) * seqs] for k in range(top)]
    total = functools.reduce(jnp.add, shares)
    mixed = functools.reduce(jnp.add, [(share / total) * value for share, value in zip(shares, values)])
    out_ref[...] = (stream_ref[...].astype(F32) + mixed).astype(BF16)


def per_device(
    residual, state_re, state_im, mix_gain, proj_in, decay_rate, frequency, log_step, input_re, input_im,
    read_re, read_im, skip_gain, glu_weight, out_proj, ffn_gain, router, gate_weight, up_weight, down_weight,
    route_ids,
):
    seqs, cols = residual.shape
    width = mix_gain.shape[0]
    peers = width // cols
    channels = skip_gain.shape[0]
    ep_size = lax.axis_size("ep")
    experts = router.shape[1]
    top = route_ids.shape[1]
    cap = seqs * top // experts + 1
    per = cap + 1
    slots = ep_size * per
    rows = ep_size * cap
    half = seqs // 2

    all_resid = exchange(jnp.broadcast_to(residual[None], (peers, seqs, cols)), TP)

    place, fetch, pick, keep, grow = call(
        functools.partial(routing_kernel, per, cap, experts),
        (
            shape_of((slots, seqs), BF16), shape_of((2 * top * seqs, slots), BF16), shape_of((top * seqs, TILE), F32),
            shape_of((rows, slots), BF16), shape_of((2, slots, rows), BF16),
        ),
        route_ids, route_ids.T,
    )
    abar_re, abar_im, bbar_re, bbar_im = discretise(
        decay_rate, frequency, log_step, input_re.transpose(0, 2, 1), input_im.transpose(0, 2, 1)
    )
    expert = lax.axis_index("ep")
    own_router = lax.dynamic_slice_in_dim(router.T, expert, 1, 0).reshape(peers, cols)
    gain = ffn_gain.reshape(peers, cols)
    all_resid, place, fetch, pick, keep, grow, own_router, gain = lax.optimization_barrier(
        (all_resid, place, fetch, pick, keep, grow, own_router, gain)
    )
    new_re, new_im, mixer, mixer_send = call(
        mixer_kernel,
        (
            shape_of(state_re.shape, F32), shape_of(state_im.shape, F32), shape_of((seqs, channels), F32),
            shape_of((peers, half, 2 * channels), BF16),
        ),
        all_resid, mix_gain.reshape(peers, cols), proj_in.T, state_re, state_im, abar_re, abar_im,
        block_diagonal(bbar_re), block_diagonal(bbar_im), block_diagonal(read_re), block_diagonal(read_im),
        skip_gain.reshape(1, channels),
    )
    all_mixer = exchange(mixer_send, TP)
    gated_send = call(
        gate_kernel, shape_of((peers, half, 2 * channels), BF16), all_mixer, glu_weight.T, mixer
    )
    all_gated = exchange(gated_send, TP)
    stream, token_send = call(
        stream_kernel,
        (shape_of((seqs, cols), BF16), shape_of((slots, cols), BF16)),
        all_gated, out_proj, residual, place,
    )
    arrived = exchange(token_send.reshape(ep_size, per // 2, 2, cols), "ep").reshape(slots, cols)
    tokens_send = call(spread_kernel, shape_of((peers, rows, cols), BF16), arrived, keep)
    tokens = exchange(tokens_send, TP)
    parts, logits = call(
        expert_kernel, (shape_of((peers, rows, cols), BF16), shape_of((rows, TILE), BF16)),
        tokens, gain, own_router, gate_weight, up_weight, down_weight, mib=24,
    )
    own_parts = exchange(parts, TP)
    back_send = call(return_kernel, shape_of((slots, cols), BF16), own_parts, grow, logits)
    back = exchange(back_send.reshape(ep_size, per // 2, 2, cols), "ep").reshape(slots, cols)
    layer_out = call(
        functools.partial(combine_kernel, top), shape_of((seqs, cols), BF16), back, fetch, pick, stream
    )
    return (layer_out, new_re, new_im)


def solution(mesh):
    split = Mesh(mesh.devices.reshape(mesh.shape["ep"], 4, 4), ("ep", "tp_0", "tp_1"))
    in_specs = (
        P("ep", TP),
        P("ep", TP, None),
        P("ep", TP, None),
        P(),
        P(None, TP),
        P(TP, None),
        P(TP, None),
        P(TP),
        P(TP, None, None),
        P(TP, None, None),
        P(TP, None, None),
        P(TP, None, None),
        P(TP),
        P(None, TP),
        P(None, TP),
        P(),
        P(),
        P("ep", None, TP),
        P("ep", None, TP),
        P("ep", TP, None),
        P("ep", None),
    )
    out_specs = (P("ep", TP), P("ep", TP, None), P("ep", TP, None))
    return jax.shard_map(
        per_device, mesh=split, in_specs=in_specs, out_specs=out_specs, check_vma=False
    )
```

```python
import functools

import jax
import jax.numpy as jnp
from jax import lax
from jax.experimental import pallas as pl
from jax.experimental.pallas import tpu as pltpu
from jax.sharding import Mesh
from jax.sharding import PartitionSpec as P

TP = ("tp_0", "tp_1")
EPSILON = 1e-05
LIMIT = 7.0
ALPHA = 1.702
F32 = jnp.float32
BF16 = jnp.bfloat16
TILE = 128
STAGGER = 9000


def call(body, out, *args, mib=16, **settings):
    return pl.pallas_call(
        body,
        out_shape=out,
        compiler_params=pltpu.CompilerParams(vmem_limit_bytes=mib << 20),
        **settings,
    )(*args)


def shape_of(shape, dtype):
    return jax.ShapeDtypeStruct(shape, dtype)


def halves(value):
    high = value.astype(BF16)
    return high, (value - high.astype(F32)).astype(BF16)


def dot(left, right):
    return jnp.dot(left, right, preferred_element_type=F32)


def dot_rows(left, right):
    return lax.dot_general(left, right, (((1,), (1,)), ((), ())), preferred_element_type=F32)


def exchange(blocks, axis):
    return lax.all_to_all(blocks, axis, 0, 0, tiled=True)


def discretise(decay_rate, frequency, log_step, input_re, input_im):
    real_part = -decay_rate
    step_size = jnp.exp(log_step)[:, None]
    magnitude = jnp.exp(step_size * real_part)
    abar_re = magnitude * jnp.cos(step_size * frequency)
    abar_im = magnitude * jnp.sin(step_size * frequency)
    denom = real_part * real_part + frequency * frequency
    minus_one = abar_re - 1.0
    coef_re = (minus_one * real_part + abar_im * frequency) / denom
    coef_im = (abar_im * real_part - minus_one * frequency) / denom
    bbar_re = coef_re[:, None] * input_re - coef_im[:, None] * input_im
    bbar_im = coef_re[:, None] * input_im + coef_im[:, None] * input_re
    return (abar_re, abar_im, bbar_re, bbar_im)


def block_diagonal(blocks):
    count, rows, cols = blocks.shape
    flat = jnp.pad(blocks.reshape(count * rows, cols), ((0, 0), (0, TILE - cols)))
    wide = jnp.concatenate([flat] * count, axis=1)
    row_block = lax.broadcasted_iota(jnp.int32, wide.shape, 0) // rows
    col_block = lax.broadcasted_iota(jnp.int32, wide.shape, 1) // TILE
    return jnp.where(row_block == col_block, wide, 0.0)


def packed(value):
    half = value.shape[0] // 2
    return jnp.concatenate([value[:half], value[half:]], axis=1)


def unpacked(ref):
    peers, half, lanes = ref.shape
    width = lanes // 2
    left = lax.broadcasted_iota(jnp.int32, (half, lanes), 1) < width
    top, bottom = [], []
    for pair in range(peers // 2):
        one = ref[2 * pair].astype(F32)
        two = ref[2 * pair + 1].astype(F32)
        top.append(jnp.where(left, one, pltpu.roll(two, width, 1)))
        bottom.append(jnp.where(left, pltpu.roll(one, width, 1), two))
    rows = [jnp.concatenate(top, axis=1), jnp.concatenate(bottom, axis=1)]
    return jnp.concatenate(rows, axis=0).astype(BF16)


def routing_kernel(per, cap, experts, route_ref, across_ref, place_ref, fetch_ref, pick_ref, keep_ref, grow_ref):
    seqs, top = route_ref.shape
    slots = place_ref.shape[0]
    rows = keep_ref.shape[0]
    route = route_ref[...]
    across = across_ref[...]

    def iota(shape, dim):
        return lax.broadcasted_iota(jnp.int32, shape, dim)

    expert_lane = iota((seqs, experts), 1)
    expert_row = iota((experts, seqs), 0)
    named = sum((route[:, k : k + 1] == expert_lane).astype(F32) for k in range(top))
    named_across = sum((across[k : k + 1, :] == expert_row).astype(F32) for k in range(top))
    earlier = (iota((seqs, seqs), 1) < iota((seqs, seqs), 0)).astype(BF16)
    earlier_across = (iota((seqs, seqs), 0) < iota((seqs, seqs), 1)).astype(BF16)
    count = dot(earlier, named.astype(BF16))
    count_across = dot(named_across.astype(BF16), earlier_across)
    slot_row = iota((slots, seqs), 0)
    slot_lane = iota((seqs, slots), 1)
    lane = iota((seqs, TILE), 1)
    place = jnp.zeros((slots, seqs), F32)
    for k in range(top):
        chosen = route[:, k : k + 1]
        slot = jnp.sum(jnp.where(chosen == expert_lane, count, 0.0), axis=1, keepdims=True).astype(jnp.int32)
        fetch_ref[k * seqs : (k + 1) * seqs, :] = (slot_lane == chosen * per + slot).astype(F32).astype(BF16)
        fetch_ref[(top + k) * seqs : (top + k + 1) * seqs, :] = (
            (slot_lane == chosen * per + cap).astype(F32).astype(BF16)
        )
        pick_ref[k * seqs : (k + 1) * seqs, :] = ((lane == slot) | (lane == slot + 16)).astype(F32)
        chosen_across = across[k : k + 1, :]
        slot_across = jnp.sum(
            jnp.where(chosen_across == expert_row, count_across, 0.0), axis=0, keepdims=True
        ).astype(jnp.int32)
        place = place + (slot_row == chosen_across * per + slot_across).astype(F32)
    place_ref[...] = place.astype(BF16)
    row = iota((rows, slots), 0)
    keep_ref[...] = (iota((rows, slots), 1) == row + ninth(row)).astype(F32).astype(BF16)
    col = iota((slots, rows), 1)
    target = iota((slots, rows), 0)
    grow_ref[0] = (target == col + ninth(col)).astype(F32).astype(BF16)
    grow_ref[1] = (target == ninth(col) * per + cap).astype(F32).astype(BF16)


def ninth(value):
    return (value * 7282) >> 16


def mixer_kernel(
    resid_ref, gain_ref, proj_ref, state_re_ref, state_im_ref, abar_re_ref, abar_im_ref,
    input_re_ref, input_im_ref, read_re_ref, read_im_ref, skip_ref,
    new_re_ref, new_im_ref, mixer_ref, send_ref,
):
    peers, seqs, cols = resid_ref.shape
    groups, entries = abar_re_ref.shape
    square = jnp.zeros((seqs, cols), F32)
    for t in range(peers):
        part = resid_ref[t].astype(F32)
        square = square + part * part
    mean = jnp.sum(square, axis=1, keepdims=True) / (peers * cols)
    scale = lax.rsqrt(mean + EPSILON)
    normed = jnp.concatenate(
        [(resid_ref[t].astype(F32) * scale * gain_ref[t : t + 1, :]).astype(BF16) for t in range(peers)], axis=1
    )
    mix = dot_rows(normed, proj_ref[...]).astype(BF16)

    def driven(ref):
        high, low = halves(ref[...])
        return dot(mix, high) + dot(mix, low)

    drive_re, drive_im = driven(input_re_ref), driven(input_im_ref)
    pad = jnp.zeros((seqs, TILE - entries), F32)
    all_re, all_im = [], []
    for g in range(groups):
        old_re, old_im = state_re_ref[:, g, :], state_im_ref[:, g, :]
        abar_re, abar_im = abar_re_ref[g : g + 1, :], abar_im_ref[g : g + 1, :]
        own = slice(g * TILE, g * TILE + entries)
        new_re = abar_re * old_re - abar_im * old_im + drive_re[:, own]
        new_im = abar_re * old_im + abar_im * old_re + drive_im[:, own]
        new_re_ref[:, g, :] = new_re
        new_im_ref[:, g, :] = new_im
        all_re += [new_re, pad]
        all_im += [new_im, pad]

    def read(values, ref):
        high, low = halves(jnp.concatenate(values, axis=1))
        read_high, read_low = halves(ref[...])
        return dot_rows(high, read_high) + dot_rows(high, read_low) + dot_rows(low, read_high)

    value = read(all_re, read_re_ref) - read(all_im, read_im_ref) + skip_ref[...] * mix.astype(F32)
    mixer = 0.5 * value * (1.0 + lax.erf(value * 0.7071067811865476))
    mixer_ref[...] = mixer
    sent = packed(mixer).astype(BF16)
    for t in range(peers):
        send_ref[t] = sent


def gate_kernel(all_ref, weight_ref, mixer_ref, send_ref):
    gate = dot_rows(unpacked(all_ref), weight_ref[...])
    gated = packed(mixer_ref[...] * jax.nn.sigmoid(gate)).astype(BF16)
    for t in range(send_ref.shape[0]):
        send_ref[t] = gated


def stream_kernel(all_ref, weight_ref, resid_ref, place_ref, stream_ref, send_ref):
    mixed = dot(unpacked(all_ref), weight_ref[...])
    stream = (resid_ref[...].astype(F32) + mixed).astype(BF16)
    stream_ref[...] = stream
    send_ref[...] = dot(place_ref[...], stream).astype(BF16)


def spread_kernel(arrived_ref, keep_ref, send_ref):
    tokens = dot(keep_ref[...], arrived_ref[...]).astype(BF16)
    for t in range(send_ref.shape[0]):
        send_ref[t] = tokens
    if STAGGER:
        @pl.when(lax.rem(lax.axis_index("ep"), 2) == 1)
        def _():
            pl.delay(STAGGER)


def expert_kernel(
    tokens_ref, gain_ref, router_ref, gate_ref, up_ref, down_ref, new_re_ref, new_im_ref,
    out_ref, logit_ref, out_re_ref, out_im_ref, sems,
):
    peers, rows, cols = tokens_ref.shape
    copies = [
        pltpu.make_async_copy(new_re_ref, out_re_ref, sems.at[0]),
        pltpu.make_async_copy(new_im_ref, out_im_ref, sems.at[1]),
    ]
    for copy in copies:
        copy.start()
    square = jnp.zeros((rows, cols), F32)
    total = jnp.zeros((rows, cols), F32)
    for t in range(peers):
        part = tokens_ref[t].astype(F32)
        square = square + part * part
        total = total + part * router_ref[t : t + 1, :]
    inverse = lax.rsqrt(jnp.sum(square, axis=1, keepdims=True) / (peers * cols) + EPSILON)
    high, low = halves(jnp.sum(total, axis=1, keepdims=True) * inverse)
    row = lax.broadcasted_iota(jnp.int32, (rows, TILE), 0)
    place = row - 9 * ninth(row)
    lane = lax.broadcasted_iota(jnp.int32, (rows, TILE), 1)
    marked = jnp.where(lane == place, high.astype(F32), 0.0) + jnp.where(lane == place + 16, low.astype(F32), 0.0)
    logit_ref[...] = marked.astype(BF16)
    normed = jnp.concatenate(
        [(tokens_ref[t].astype(F32) * inverse * gain_ref[t : t + 1, :]).astype(BF16) for t in range(peers)], axis=1
    )
    gate = jnp.minimum(dot(normed, gate_ref[0]), LIMIT)
    up = jnp.clip(dot(normed, up_ref[0]), -LIMIT, LIMIT)
    active = ((up + 1.0) * (gate * jax.nn.sigmoid(ALPHA * gate))).astype(BF16)
    for t in range(0, peers, 2):
        part = dot(active, down_ref[0, :, t * cols : (t + 2) * cols]).astype(BF16)
        out_ref[t] = part[:, :cols]
        out_ref[t + 1] = part[:, cols:]
    for copy in copies:
        copy.wait()


def return_kernel(parts_ref, grow_ref, logits_ref, send_ref):
    total = parts_ref[0].astype(F32)
    for t in range(1, parts_ref.shape[0]):
        total = total + parts_ref[t].astype(F32)
    grown = dot(grow_ref[0], total.astype(BF16)) + dot(grow_ref[1], logits_ref[...])
    send_ref[...] = grown.astype(BF16)


def combine_kernel(top, back_ref, fetch_ref, pick_ref, stream_ref, out_ref):
    fetched = dot(fetch_ref[...], back_ref[...])
    seqs = stream_ref.shape[0]
    half = top * seqs
    picked = jnp.sum(fetched[half:] * pick_ref[...], axis=1, keepdims=True)
    expon = jnp.exp(picked)
    values = [fetched[k * seqs : (k + 1) * seqs] for k in range(top)]
    shares = [expon[k * seqs : (k + 1) * seqs] for k in range(top)]
    total = functools.reduce(jnp.add, shares)
    mixed = functools.reduce(jnp.add, [(share / total) * value for share, value in zip(shares, values)])
    out_ref[...] = (stream_ref[...].astype(F32) + mixed).astype(BF16)


def per_device(
    residual, state_re, state_im, mix_gain, proj_in, decay_rate, frequency, log_step, input_re, input_im,
    read_re, read_im, skip_gain, glu_weight, out_proj, ffn_gain, router, gate_weight, up_weight, down_weight,
    route_ids,
):
    seqs, cols = residual.shape
    width = mix_gain.shape[0]
    peers = width // cols
    channels = skip_gain.shape[0]
    ep_size = lax.axis_size("ep")
    experts = router.shape[1]
    top = route_ids.shape[1]
    cap = seqs * top // experts + 1
    per = cap + 1
    slots = ep_size * per
    rows = ep_size * cap
    half = seqs // 2

    all_resid = exchange(jnp.broadcast_to(residual[None], (peers, seqs, cols)), TP)

    place, fetch, pick, keep, grow = call(
        functools.partial(routing_kernel, per, cap, experts),
        (
            shape_of((slots, seqs), BF16), shape_of((2 * top * seqs, slots), BF16), shape_of((top * seqs, TILE), F32),
            shape_of((rows, slots), BF16), shape_of((2, slots, rows), BF16),
        ),
        route_ids, route_ids.T,
    )
    abar_re, abar_im, bbar_re, bbar_im = discretise(
        decay_rate, frequency, log_step, input_re.transpose(0, 2, 1), input_im.transpose(0, 2, 1)
    )
    expert = lax.axis_index("ep")
    gain = ffn_gain.reshape(peers, cols)
    own_router = lax.dynamic_slice_in_dim(router.T, expert, 1, 0).reshape(peers, cols) * gain
    all_resid, place, fetch, pick, keep, grow, own_router, gain = lax.optimization_barrier(
        (all_resid, place, fetch, pick, keep, grow, own_router, gain)
    )
    new_re, new_im, mixer, mixer_send = call(
        mixer_kernel,
        (
            shape_of(state_re.shape, F32), shape_of(state_im.shape, F32), shape_of((seqs, channels), F32),
            shape_of((peers, half, 2 * channels), BF16),
        ),
        all_resid, mix_gain.reshape(peers, cols), proj_in.T, state_re, state_im, abar_re, abar_im,
        block_diagonal(bbar_re), block_diagonal(bbar_im), block_diagonal(read_re), block_diagonal(read_im),
        skip_gain.reshape(1, channels),
    )
    all_mixer = exchange(mixer_send, TP)
    gated_send = call(
        gate_kernel, shape_of((peers, half, 2 * channels), BF16), all_mixer, glu_weight.T, mixer
    )
    all_gated = exchange(gated_send, TP)
    stream, token_send = call(
        stream_kernel,
        (shape_of((seqs, cols), BF16), shape_of((slots, cols), BF16)),
        all_gated, out_proj, residual, place,
    )
    arrived = exchange(token_send.reshape(ep_size, per // 2, 2, cols), "ep").reshape(slots, cols)
    tokens_send = call(spread_kernel, shape_of((peers, rows, cols), BF16), arrived, keep)
    tokens = exchange(tokens_send, TP)
    far, near = pl.BlockSpec(memory_space=pl.ANY), pl.BlockSpec(memory_space=pltpu.VMEM)
    parts, logits, out_re, out_im = call(
        expert_kernel,
        (
            shape_of((peers, rows, cols), BF16), shape_of((rows, TILE), BF16),
            shape_of(state_re.shape, F32), shape_of(state_im.shape, F32),
        ),
        tokens, gain, own_router, gate_weight, up_weight, down_weight, new_re, new_im, mib=24,
        out_specs=(near, near, far, far), scratch_shapes=[pltpu.SemaphoreType.DMA((2,))],
    )
    own_parts = exchange(parts, TP)
    back_send = call(return_kernel, shape_of((slots, cols), BF16), own_parts, grow, logits)
    back = exchange(back_send.reshape(ep_size, per // 2, 2, cols), "ep").reshape(slots, cols)
    layer_out = call(
        functools.partial(combine_kernel, top), shape_of((seqs, cols), BF16), back, fetch, pick, stream
    )
    return (layer_out, out_re, out_im)


def solution(mesh):
    split = Mesh(mesh.devices.reshape(mesh.shape["ep"], 4, 4), ("ep", "tp_0", "tp_1"))
    in_specs = (
        P("ep", TP),
        P("ep", TP, None),
        P("ep", TP, None),
        P(),
        P(None, TP),
        P(TP, None),
        P(TP, None),
        P(TP),
        P(TP, None, None),
        P(TP, None, None),
        P(TP, None, None),
        P(TP, None, None),
        P(TP),
        P(None, TP),
        P(None, TP),
        P(),
        P(),
        P("ep", None, TP),
        P("ep", None, TP),
        P("ep", TP, None),
        P("ep", None),
    )
    out_specs = (P("ep", TP), P("ep", TP, None), P("ep", TP, None))
    return jax.shard_map(
        per_device, mesh=split, in_specs=in_specs, out_specs=out_specs, check_vma=False
    )
```
